32 devices in a mesh: fs: 4 (over z), tp: 8 (over y, x, core).
Axes of the slice: x: 2, y: 2, z: 4, core: 2. Of those that a mesh axis runs over, the one named last changes fastest.
Arguments:
- block_in: bfloat16 [4096, 2304], P('fs'), may hold values from -6 to 6
- out_cot: bfloat16 [4096, 2304], P('fs'), may hold values from -6 to 6
- gated_out: bfloat16 [4096, 4608], P('fs', 'tp'), may hold values from -6 to 6
- gate_cot: bfloat16 [4096, 4608], P('fs', 'tp'), may hold values from -6 to 6
- factor_out: bfloat16 [2304, 192], P('fs'), may hold values from -0.104166667 to 0.104166667
- factor_z: bfloat16 [2304, 192], P('fs'), may hold values from -0.104166667 to 0.104166667
- weight_out: float32 [4608, 2304], P('tp', 'fs'), may hold values from -0.09375 to 0.09375
- weight_z: float32 [2304, 4608], P('fs', 'tp'), may hold values from -0.125 to 0.125
- first_out: float32 [4608, 192], P('tp', 'fs'), may hold values from -512 to 512
- second_out: float32 [4608, 192], P('tp', 'fs'), may hold values from 819.2 to 20480
- first_z: float32 [192, 4608], P('fs', 'tp'), may hold values from -512 to 512
- second_z: float32 [192, 4608], P('fs', 'tp'), may hold values from 819.2 to 20480
Outputs:
- step_out: float32 [4608, 2304], P('tp', 'fs')
- step_z: float32 [2304, 4608], P('fs', 'tp')
- new_first_out: float32 [4608, 192], P('tp', 'fs')
- new_second_out: float32 [4608, 192], P('tp', 'fs')
- new_first_z: float32 [192, 4608], P('fs', 'tp')
- new_second_z: float32 [192, 4608], P('fs', 'tp')
- copy_out: bfloat16 [4608, 2304], P('tp')
- copy_z: bfloat16 [2304, 4608], P(None, 'tp')
The draws below stay inside these ranges and needn't reach their ends.
All inputs are finite; a program needn't handle non-finite values.
Results may differ from the reference program's by a relative error of at most 0.0018.
Values may be sent and summed in bfloat16 or wider, within the bound.
A program may use at most 64 MiB of HBM per device.

```python
import math
import jax
import jax.numpy as jnp
from jax import lax

D = 2304
INNER = 4608
RANK = 192
TOKENS = 4096


def shared_parts(key, member):
    folded = jax.random.fold_in(key, 1000 + member)
    subkeys = jax.random.split(folded, 4)
    width_dir = jnp.clip(jax.random.normal(subkeys[0], (D,), jnp.float32), -3.0, 3.0)
    inner_dir = jnp.clip(jax.random.normal(subkeys[1], (INNER,), jnp.float32), -3.0, 3.0)
    rank_wts = jax.random.uniform(subkeys[2], (RANK,), jnp.float32, 0.5, 1.5)
    token_sign = (2 * jax.random.randint(subkeys[3], (TOKENS,), 0, 2) - 1).astype(jnp.float32)
    return (width_dir, inner_dir, rank_wts, token_sign)


def noise_field(key, label_code, array_shape, clip_bound):
    subkey = jax.random.fold_in(key, label_code)
    return jnp.clip(jax.random.normal(subkey, array_shape, jnp.float32), -clip_bound, clip_bound)


def coupling_level():
    return min(math.sqrt(15.0 / math.sqrt(D * TOKENS)), 0.5)


def token_field(key, member, label_code, use_width):
    width_dir, inner_dir, rank_wts, token_sign = shared_parts(key, member)
    if use_width:
        common_dir = width_dir
        columns = D
    else:
        common_dir = inner_dir
        columns = INNER
    drawn = noise_field(key, label_code, (TOKENS, columns), 4.0)
    drawn = drawn + coupling_level() * token_sign[:, None] * common_dir[None, :]
    return jnp.clip(drawn, -6.0, 6.0).astype(jnp.bfloat16)


def factor_field(key, member, label_code):
    width_dir, inner_dir, rank_wts, token_sign = shared_parts(key, member)
    spread = D ** (-0.5)
    drawn = spread * noise_field(key, label_code, (D, RANK), 4.0)
    drawn = drawn + 0.1 * spread * width_dir[:, None] * rank_wts[None, :]
    return jnp.clip(drawn, -5.0 * spread, 5.0 * spread).astype(jnp.bfloat16)


def draw_block_in(key, part):
    return token_field(key, 2, 11, True)


def draw_gate_cot(key, part):
    return token_field(key, 2, 12, False)


def draw_out_cot(key, part):
    return token_field(key, 1, 13, True)


def draw_gated_out(key, part):
    return token_field(key, 1, 14, False)


def draw_factor_out(key, part):
    return factor_field(key, 1, 15)


def draw_factor_z(key, part):
    return factor_field(key, 2, 16)


def draw_first_out(key, part):
    width_dir, inner_dir, rank_wts, token_sign = shared_parts(key, 1)
    root_tokens = math.sqrt(TOKENS)
    drawn = noise_field(key, 17, (INNER, RANK), 4.0) + 0.8 * inner_dir[:, None] * rank_wts[None, :]
    return jnp.clip(root_tokens * drawn, -8.0 * root_tokens, 8.0 * root_tokens)


def draw_first_z(key, part):
    width_dir, inner_dir, rank_wts, token_sign = shared_parts(key, 2)
    root_tokens = math.sqrt(TOKENS)
    drawn = noise_field(key, 18, (RANK, INNER), 4.0) + 0.8 * rank_wts[:, None] * inner_dir[None, :]
    return jnp.clip(root_tokens * drawn, -8.0 * root_tokens, 8.0 * root_tokens)


def level_of(own_key, extent, pieces, low, high):
    loudness, own = 1.0, jax.random.fold_in(own_key, 6)
    for position, blocks in pieces:
        draws = jnp.exp(jax.random.uniform(jax.random.fold_in(own, position), (blocks,), jnp.float32, low / len(pieces), high / len(pieces)))
        loudness = loudness * jnp.repeat(draws, extent[position] // blocks).reshape([-1 if axis == position else 1 for axis in range(len(extent))])
    return loudness


def scatter_about(own_key, dims, scale, reach, cuts=(), kind=jnp.bfloat16):
    result = scale * jax.random.normal(own_key, dims, jnp.float32)
    if cuts:
        result = result * level_of(own_key, dims, cuts, -0.22, 0.18)
    return jnp.clip(result, -reach, reach).astype(kind)


def setup_inputs(seed: int = 0) -> dict:
    key_list = jax.random.split(jax.random.key(seed), 13)
    return {
        "block_in": draw_block_in(jax.random.fold_in(key_list[12], 71), 0),
        "out_cot": draw_out_cot(jax.random.fold_in(key_list[12], 71), 0),
        "gated_out": draw_gated_out(jax.random.fold_in(key_list[12], 71), 0),
        "gate_cot": draw_gate_cot(jax.random.fold_in(key_list[12], 71), 0),
        "factor_out": draw_factor_out(jax.random.fold_in(key_list[12], 71), 0),
        "factor_z": draw_factor_z(jax.random.fold_in(key_list[12], 71), 0),
        "weight_out": scatter_about(key_list[6], (INNER, D), INNER ** -0.5, 0.09375, ((0, 8), (1, 4)), jnp.float32),
        "weight_z": scatter_about(key_list[7], (D, INNER), D ** -0.5, 0.125, ((0, 4), (1, 8)), jnp.float32),
        "first_out": draw_first_out(jax.random.fold_in(key_list[12], 71), 0),
        "second_out": jnp.clip(jnp.exp(math.log(20480.0) - 3.218876 * jax.random.uniform(key_list[9], (INNER, RANK), jnp.float32) ** level_of(key_list[9], (INNER, RANK), ((0, 8), (1, 4)), -0.2, 0.2)), 819.2, 20480.0),
        "first_z": draw_first_z(jax.random.fold_in(key_list[12], 71), 0),
        "second_z": jnp.clip(jnp.exp(math.log(20480.0) - 3.218876 * jax.random.uniform(key_list[11], (RANK, INNER), jnp.float32) ** level_of(key_list[11], (RANK, INNER), ((0, 4), (1, 8)), -0.2, 0.2)), 819.2, 20480.0),
    }


beta_first = 0.8
beta_second = 0.9
adam_eps = 1e-08
norm_eps = 1e-06
rate = 0.005

def moments(first, second, gradient):
    new_first = beta_first * first + (1.0 - beta_first) * gradient
    new_second = beta_second * second + (1.0 - beta_second) * gradient * gradient
    return (new_first, new_second, new_first / (jnp.sqrt(new_second) + adam_eps))

def reference(block_in, out_cot, gated_out, gate_cot, factor_out, factor_z, weight_out, weight_z, first_out, second_out, first_z, second_z):
    proj_cot = jnp.dot(out_cot.astype(jnp.float32), factor_out.astype(jnp.float32), precision=lax.Precision.HIGHEST)
    proj_input = jnp.dot(block_in.astype(jnp.float32), factor_z.astype(jnp.float32), precision=lax.Precision.HIGHEST)
    grad_out = jnp.dot(gated_out.astype(jnp.float32).T, proj_cot, precision=lax.Precision.HIGHEST)
    grad_z = jnp.dot(proj_input.T, gate_cot.astype(jnp.float32), precision=lax.Precision.HIGHEST)
    new_first_out, new_second_out, dir_out = moments(first_out, second_out, grad_out)
    new_first_z, new_second_z, dir_z = moments(first_z, second_z, grad_z)
    update_out = jnp.dot(dir_out, factor_out.astype(jnp.float32).T, precision=lax.Precision.HIGHEST)
    update_z = jnp.dot(factor_z.astype(jnp.float32), dir_z, precision=lax.Precision.HIGHEST)
    step_out = update_out * lax.rsqrt(jnp.mean(update_out * update_out) + norm_eps)
    step_z = update_z * lax.rsqrt(jnp.mean(update_z * update_z) + norm_eps)
    copy_out = (weight_out - rate * step_out).astype(jnp.bfloat16)
    copy_z = (weight_z - rate * step_z).astype(jnp.bfloat16)
    return (step_out, step_z, new_first_out, new_second_out, new_first_z, new_second_z, copy_out, copy_z)
```

```python
import functools
import math

import jax
import jax.numpy as jnp
from jax import lax
from jax.experimental import pallas as pl
from jax.experimental.pallas import tpu as pltpu
from jax.sharding import PartitionSpec as P

beta_first = 0.8
beta_second = 0.9
adam_eps = 1e-08
norm_eps = 1e-06
rate = 0.005

MESH = pl.DeviceIdType.MESH
VMEM = pl.BlockSpec(memory_space=pltpu.VMEM)
ANY = pl.BlockSpec(memory_space=pl.ANY)
PARTS = 8
SPAN = 120.0 * math.log(2.0)
WEIGHT_BOUND = 0.125
DIR_BOUND = 16.0
VALUE_BOUND = 6.0
FACTOR_BOUND = 0.104166667

f32, bf16 = jnp.float32, jnp.bfloat16


def remote(src, dst, send, recv, **where):
    return pltpu.make_async_remote_copy(
        src_ref=src, dst_ref=dst, send_sem=send, recv_sem=recv, device_id=where, device_id_type=MESH
    )


def encode(values, bound, roots):
    size = jnp.abs(values) * (1.0 / bound)
    for _ in range(roots):
        size = jnp.sqrt(size)
    code = jnp.exp(size * (2.0 * SPAN) - SPAN)
    return jnp.where(values < 0.0, -code, code).astype(bf16)


def decode(code, bound, roots):
    code = code.astype(f32)
    size = (jnp.log(jnp.abs(code)) + SPAN) * (0.5 / SPAN)
    for _ in range(roots):
        size = size * size
    size = size * bound
    return jnp.where(code < 0.0, -size, size)


def split(values):
    high = values.astype(bf16)
    return high, (values - high.astype(f32)).astype(bf16)


def nn(a, b):
    return jnp.dot(a, b, preferred_element_type=f32)


def nt(a, b):
    return lax.dot_general(a, b, (((1,), (1,)), ((), ())), preferred_element_type=f32)


def tn(a, b):
    return lax.dot_general(a, b, (((0,), (0,)), ((), ())), preferred_element_type=f32)


def flip(index, bit):
    return index + bit - 2 * bit * lax.rem(index // bit, 2)


def main_kernel(
    fs, tp, chunks, grad_bound,
    out_cot, block_in, gated, gate, factor_out, factor_z, weight_out, weight_z,
    first_out, second_out, first_z, second_z,
    copy_out, copy_z, step_out, step_z, new_first_out, new_second_out, new_first_z, new_second_z,
    tokens_v, inner_v, wo_v, wz_v, wt_v, moments_v,
    full, wall, joined, term, term_code, arrived, dir_code, dir_t, dir_n, update,
    partial, received,
    load, send_f, recv_f, send_p, recv_p, send_u, recv_u, send_d, recv_d,
    send_r, recv_r, send_g, recv_g, send_t, recv_t,
):
    me, mine = lax.axis_index("fs"), lax.axis_index("tp")
    inner, width = weight_out.shape
    rank = factor_out.shape[0]
    share = rank // fs
    tokens = out_cot.shape[0]
    rows = inner // chunks
    entries = float(width * fs * inner * tp)
    part = lax.rem(mine, PARTS)
    piece = 2 * rank // PARTS

    loads = []

    def fetch(src, dst):
        copy = pltpu.make_async_copy(src, dst, load.at[len(loads)])
        copy.start()
        loads.append(copy)
        return copy

    in_factor = [
        fetch(factor_out, full.at[me, pl.ds(0, rank)]),
        fetch(factor_z, full.at[me, pl.ds(rank, rank)]),
    ]
    in_weight = [fetch(weight_out, wo_v), fetch(weight_z, wz_v)]
    in_tokens = [
        (fetch(out_cot, tokens_v.at[0]), fetch(gated, inner_v.at[0])),
        (fetch(block_in, tokens_v.at[1]), fetch(gate, inner_v.at[1])),
    ]
    in_moments = [
        fetch(ref, moments_v.at[i]) for i, ref in enumerate((first_out, first_z, second_out, second_z))
    ]

    barrier = pltpu.get_barrier_semaphore()
    for d in range(1, fs):
        pl.semaphore_signal(barrier, inc=1, device_id={"fs": lax.rem(me + d, fs)}, device_id_type=MESH)
    for d in range(1, tp):
        pl.semaphore_signal(barrier, inc=1, device_id={"tp": lax.rem(mine + d, tp)}, device_id_type=MESH)

    for copy in in_weight:
        copy.wait()
    wt_v[...] = wz_v[...].T

    def pack(r, _):
        at = pl.ds(pl.multiple_of(r * 16, 16), 16)
        pair = jnp.concatenate([wo_v[at, :], wt_v[at, :]], axis=1)
        wall[me, at, :] = encode(pair, WEIGHT_BOUND, 1)
        return 0

    lax.fori_loop(0, inner // 16, pack, 0)
    for copy in in_factor:
        copy.wait()
    pl.semaphore_wait(barrier, fs + tp - 2)

    def piece_of(src, p):
        return full.at[src, pl.ds(pl.multiple_of(p * piece, piece), piece)]

    spread = []
    for d in range(1, fs):
        block = piece_of(me, part)
        copy = remote(block, block, send_f.at[d - 1], recv_f.at[d - 1], fs=lax.rem(me + d, fs))
        copy.start()
        spread.append(copy)

    def chunk_of(src, c):
        return wall.at[src, pl.ds(pl.multiple_of(c * rows, rows), rows)]

    def up(h, c):
        block = chunk_of(jnp.maximum(me - h, 0), c)
        return remote(block, block, send_u.at[h, c], recv_u.at[h, c], fs=jnp.minimum(me + 1, fs - 1))

    def down(h, c):
        block = chunk_of(jnp.minimum(me + h, fs - 1), c)
        return remote(block, block, send_d.at[h, c], recv_d.at[h, c], fs=jnp.maximum(me - 1, 0))

    def start_own(c, _):
        @pl.when(me < fs - 1)
        def _():
            up(0, c).start()

        @pl.when(me > 0)
        def _():
            down(0, c).start()

        return 0

    lax.fori_loop(0, chunks, start_own, 0)

    def pump(h):
        def body(c, _):
            @pl.when((me - h >= 0) & (me < fs - 1))
            def _():
                up(h - 1, c).wait_recv()
                up(h, c).start()

            @pl.when((me + h < fs) & (me > 0))
            def _():
                down(h - 1, c).wait_recv()
                down(h, c).start()

            return 0

        lax.fori_loop(0, chunks, body, 0)

    plane = []

    def pass_on(d, k, p, bit):
        block = piece_of(lax.rem(me - d + fs, fs), p)
        copy = remote(block, block, send_p.at[d - 1, k], recv_p.at[d - 1, k], tp=flip(mine, bit))
        copy.start()
        plane.append(copy)
        return copy

    by_y, by_x = [], []
    for d in range(1, fs):
        spread[d - 1].wait_recv()
        by_y.append(pass_on(d, 0, part, 4))
        by_x.append([pass_on(d, 1, part, 2)])
        pass_on(d, 3, part, 1)
    for d in range(1, fs):
        by_y[d - 1].wait_recv()
        by_x[d - 1].append(pass_on(d, 2, flip(part, 4), 2))
        pass_on(d, 4, flip(part, 4), 1)
    for d in range(1, fs):
        for k, copy in enumerate(by_x[d - 1]):
            copy.wait_recv()
            p = flip(part, 2)
            pass_on(d, 5 + k, p if k == 0 else flip(p, 4), 1)
    waited = [c for c in by_y] + [c for pair in by_x for c in pair]
    for copy in plane:
        if not any(copy is other for other in waited):
            copy.wait_recv()

    block_t = 256 if tokens % 256 == 0 else tokens
    for m in range(2):
        joined[m] = jnp.concatenate(
            [full[s, pl.ds(m * rank, rank), :] for s in range(fs)], axis=1
        )
        for copy in in_tokens[m]:
            copy.wait()

        def project(c, _, m=m):
            at = pl.ds(pl.multiple_of(c * block_t, block_t), block_t)
            high, low = split(nt(joined[m], tokens_v[m, at, :]))
            other = inner_v[m, :, at]
            value = nt(high, other) + nt(low, other)
            term[m] = jnp.where(c == 0, value, term[m] + value)
            return 0

        term[m] = jnp.zeros((rank, inner), f32)
        lax.fori_loop(0, tokens // block_t, project, 0)

    for s in range(fs):
        at = pl.ds(s * share, share)
        term_code[s] = encode(
            jnp.concatenate([term[0, at, :], term[1, at, :]], axis=1), grad_bound, 4
        )
    if fs > 2:
        pump(1)
    sums = []
    for d in range(1, fs):
        peer = lax.rem(me + d, fs)
        copy = remote(term_code.at[peer], arrived.at[d - 1], send_r.at[d - 1], recv_r.at[d - 1], fs=peer)
        copy.start()
        sums.append(copy)
    for copy in in_moments:
        copy.wait()
    own = pl.ds(pl.multiple_of(me * share, share), share)
    gradient = jnp.concatenate([term[0, own, :], term[1, own, :]], axis=1)
    for d in range(1, fs):
        sums[d - 1].wait_recv()
        gradient = gradient + decode(arrived[d - 1], grad_bound, 4)
    first = jnp.concatenate([moments_v[0], moments_v[1]], axis=1)
    second = jnp.concatenate([moments_v[2], moments_v[3]], axis=1)
    moment = beta_first * first + (1.0 - beta_first) * gradient
    square = beta_second * second + (1.0 - beta_second) * gradient * gradient
    dir_code[me] = encode(moment / (jnp.sqrt(square) + adam_eps), DIR_BOUND, 3)
    new_first_out[...] = moment[:, :inner]
    new_first_z[...] = moment[:, inner:]
    new_second_out[...] = square[:, :inner]
    new_second_z[...] = square[:, inner:]
    gathers = []
    for d in range(1, fs):
        block = dir_code.at[me]
        copy = remote(block, block, send_g.at[d - 1], recv_g.at[d - 1], fs=lax.rem(me + d, fs))
        copy.start()
        gathers.append(copy)
    for h in range(2, fs - 1):
        pump(h)
    for copy in gathers:
        copy.wait_recv()

    whole = decode(jnp.concatenate([dir_code[s] for s in range(fs)], axis=0), DIR_BOUND, 3)
    for m in range(2):
        values = whole[:, m * inner:(m + 1) * inner]
        high, low = split(values.T)
        dir_t[m, 0] = high
        dir_t[m, 1] = low
    high, low = split(whole[:, inner:])
    dir_n[0] = high
    dir_n[1] = low

    squares = []
    for m in range(2):
        def grow(c, acc, m=m):
            at = pl.ds(pl.multiple_of(c * rows, rows), rows)
            value = nn(dir_t[m, 0, at, :], joined[m]) + nn(dir_t[m, 1, at, :], joined[m])
            update[m, at, :] = value
            return acc + jnp.sum(value * value, axis=0, keepdims=True)

        acc = lax.fori_loop(0, chunks, grow, jnp.zeros((1, fs * width), f32))
        squares.append(jnp.sum(acc))
    row = lax.broadcasted_iota(jnp.int32, partial.shape, 0)
    partial[...] = jnp.where(row == 0, squares[0], squares[1])
    own_z = full[me, pl.ds(rank, rank), :]
    step_z[...] = tn(own_z, dir_n[0]) + tn(own_z, dir_n[1])
    totals = []
    for d in range(1, tp):
        copy = remote(
            partial, received.at[d - 1], send_t.at[d - 1], recv_t.at[d - 1], tp=lax.rem(mine + d, tp)
        )
        copy.start()
        totals.append(copy)
    own_out = full[me, pl.ds(0, rank), :]
    step_out[...] = nn(dir_t[0, 0], own_out) + nn(dir_t[0, 1], own_out)
    result = partial[...]
    for d in range(1, tp):
        totals[d - 1].wait_recv()
        result = result + received[d - 1]
    scale = lax.rsqrt(result * (1.0 / entries) + norm_eps)
    scale_out, scale_z = scale[0:1, 0:1], scale[1:2, 0:1]
    step_out[...] = step_out[...] * scale_out
    step_z[...] = step_z[...] * scale_z

    def finish(c, _):
        @pl.when(me == fs - 1)
        def _():
            for h in range(fs - 1):
                up(h, c).wait_recv()

        @pl.when(me == 0)
        def _():
            for h in range(fs - 1):
                down(h, c).wait_recv()

        def fresh(r, _):
            at = pl.ds(pl.multiple_of(c * rows + r * 16, 16), 16)
            for m, (dst, size) in enumerate(((copy_out, scale_out), (copy_z, scale_z))):
                code = jnp.concatenate(
                    [wall[s, at, m * width:(m + 1) * width] for s in range(fs)], axis=1
                )
                step = update[m, at, :] * size
                dst[at, :] = (decode(code, WEIGHT_BOUND, 1) - rate * step).astype(bf16)
            return 0

        lax.fori_loop(0, rows // 16, fresh, 0)
        return 0

    lax.fori_loop(0, chunks, finish, 0)

    for h in range(fs - 1):
        def drain(c, _, h=h):
            @pl.when((me - h >= 0) & (me < fs - 1))
            def _():
                up(h, c).wait_send()

            @pl.when((me + h < fs) & (me > 0))
            def _():
                down(h, c).wait_send()

            return 0

        lax.fori_loop(0, chunks, drain, 0)
    for copy in spread + plane + sums + gathers + totals:
        copy.wait_send()


def store_kernel(*refs):
    count = (len(refs) - 1) // 2
    sems = refs[-1]
    copies = [
        pltpu.make_async_copy(refs[i], refs[count + i], sems.at[i]) for i in range(count)
    ]
    for copy in copies:
        copy.start()
    for copy in copies:
        copy.wait()


def per_device(
    fs, tp,
    block_in, out_cot, gated_out, gate_cot, factor_out, factor_z,
    weight_out, weight_z, first_out, second_out, first_z, second_z,
):
    width, rank = factor_out.shape
    tokens, inner = gated_out.shape
    share = rank // fs
    chunks = next(n for n in (6, 3, 2, 1) if inner % (16 * n) == 0)
    grad_bound = 2.0 ** math.ceil(
        math.log2(tokens * VALUE_BOUND * width * fs * VALUE_BOUND * FACTOR_BOUND)
    )
    dma = pltpu.SemaphoreType.DMA
    shape = jax.ShapeDtypeStruct
    moment = shape((share, inner), f32)
    results = (
        shape((inner, fs * width), bf16),
        shape((inner, fs * width), bf16),
        shape((inner, width), f32),
        shape((width, inner), f32),
        moment, moment, moment, moment,
    )
    hops = dma((fs - 1, chunks))
    peers = dma((fs - 1,))
    others = dma((tp - 1,))
    pieces = dma((fs - 1, PARTS - 1))
    made = pl.pallas_call(
        functools.partial(main_kernel, fs, tp, chunks, grad_bound),
        out_shape=results,
        in_specs=[ANY] * 12,
        out_specs=[VMEM] * 8,
        scratch_shapes=[
            pltpu.VMEM((2, tokens, fs * width), bf16),
            pltpu.VMEM((2, inner, tokens), bf16),
            pltpu.VMEM((inner, width), f32),
            pltpu.VMEM((width, inner), f32),
            pltpu.VMEM((inner, width), f32),
            pltpu.VMEM((4, share, inner), f32),
            pltpu.VMEM((fs, 2 * rank, width), bf16),
            pltpu.VMEM((fs, inner, 2 * width), bf16),
            pltpu.VMEM((2, rank, fs * width), bf16),
            pltpu.VMEM((2, rank, inner), f32),
            pltpu.VMEM((fs, share, 2 * inner), bf16),
            pltpu.VMEM((fs - 1, share, 2 * inner), bf16),
            pltpu.VMEM((fs, share, 2 * inner), bf16),
            pltpu.VMEM((2, 2, inner, rank), bf16),
            pltpu.VMEM((2, rank, inner), bf16),
            pltpu.VMEM((2, inner, fs * width), f32),
            pltpu.VMEM((8, 128), f32),
            pltpu.VMEM((tp - 1, 8, 128), f32),
            dma((12,)),
            peers, peers, pieces, pieces, hops, hops, hops, hops,
            peers, peers, peers, peers, others, others,
        ],
        compiler_params=pltpu.CompilerParams(
            collective_id=0, has_side_effects=True, vmem_limit_bytes=52 * 1024 * 1024
        ),
        cost_estimate=pl.CostEstimate(flops=10**10, bytes_accessed=30_000_000, transcendentals=0),
    )(
        out_cot, block_in, gated_out.T, gate_cot.T, factor_out.T, factor_z.T, weight_out, weight_z,
        first_out.T, second_out.T, first_z, second_z,
    )
    kept = pl.pallas_call(
        store_kernel,
        out_shape=results,
        in_specs=[VMEM] * 8,
        out_specs=[ANY] * 8,
        scratch_shapes=[dma((8,))],
        cost_estimate=pl.CostEstimate(flops=10**6, bytes_accessed=20_000_000, transcendentals=0),
    )(*made)
    copy_out, copy_z, step_out, step_z, nf_out, ns_out, nf_z, ns_z = kept
    return step_out, step_z, nf_out.T, ns_out.T, nf_z, ns_z, copy_out, copy_z.T


def solution(mesh):
    return jax.shard_map(
        functools.partial(per_device, mesh.shape["fs"], mesh.shape["tp"]),
        mesh=mesh,
        in_specs=(
            P("fs", None),
            P("fs", None),
            P("fs", "tp"),
            P("fs", "tp"),
            P("fs", None),
            P("fs", None),
            P("tp", "fs"),
            P("fs", "tp"),
            P("tp", "fs"),
            P("tp", "fs"),
            P("fs", "tp"),
            P("fs", "tp"),
        ),
        out_specs=(
            P("tp", "fs"),
            P("fs", "tp"),
            P("tp", "fs"),
            P("tp", "fs"),
            P("fs", "tp"),
            P("fs", "tp"),
            P("tp", None),
            P(None, "tp"),
        ),
        check_vma=False,
    )
```

```python
import functools
import math

import jax
import jax.numpy as jnp
from jax import lax
from jax.experimental import pallas as pl
from jax.experimental.pallas import tpu as pltpu
from jax.sharding import PartitionSpec as P

beta_first = 0.8
beta_second = 0.9
adam_eps = 1e-08
norm_eps = 1e-06
rate = 0.005

MESH = pl.DeviceIdType.MESH
VMEM = pl.BlockSpec(memory_space=pltpu.VMEM)
ANY = pl.BlockSpec(memory_space=pl.ANY)
PARTS = 8
SPAN = 120.0 * math.log(2.0)
WEIGHT_BOUND = 0.125
DIR_BOUND = 16.0
VALUE_BOUND = 6.0
FACTOR_BOUND = 0.104166667

f32, bf16 = jnp.float32, jnp.bfloat16


def remote(src, dst, send, recv, **where):
    return pltpu.make_async_remote_copy(
        src_ref=src, dst_ref=dst, send_sem=send, recv_sem=recv, device_id=where, device_id_type=MESH
    )


def encode(values, bound, roots):
    size = jnp.abs(values) * (1.0 / bound)
    for _ in range(roots):
        size = jnp.sqrt(size)
    code = jnp.exp(size * (2.0 * SPAN) - SPAN)
    return jnp.where(values < 0.0, -code, code).astype(bf16)


def decode(code, bound, roots):
    code = code.astype(f32)
    size = (jnp.log(jnp.abs(code)) + SPAN) * (0.5 / SPAN)
    for _ in range(roots):
        size = size * size
    size = size * bound
    return jnp.where(code < 0.0, -size, size)


def split(values):
    high = values.astype(bf16)
    return high, (values - high.astype(f32)).astype(bf16)


def nn(a, b):
    return jnp.dot(a, b, preferred_element_type=f32)


def nt(a, b):
    return lax.dot_general(a, b, (((1,), (1,)), ((), ())), preferred_element_type=f32)


def tn(a, b):
    return lax.dot_general(a, b, (((0,), (0,)), ((), ())), preferred_element_type=f32)


def flip(index, bit):
    return index + bit - 2 * bit * lax.rem(index // bit, 2)


def main_kernel(
    fs, tp, chunks, grad_bound,
    out_cot, block_in, gated, gate, factor_out, factor_z, weight_out, weight_z,
    first_out, second_out, first_z, second_z,
    copy_out, copy_z, step_out, step_z, new_first_out, new_second_out, new_first_z, new_second_z,
    tokens_v, inner_v, wo_v, wz_v, wt_v, moments_v,
    full, wall, joined, term, rise_out, rise_in, fall_out, fall_in, sum_v, dir_code, dir_t, dir_n, update,
    partial, received,
    load, send_f, recv_f, send_p, recv_p, send_u, recv_u, send_d, recv_d,
    send_r, recv_r, send_g, recv_g, send_t, recv_t,
):
    me, mine = lax.axis_index("fs"), lax.axis_index("tp")
    inner, width = weight_out.shape
    rank = factor_out.shape[0]
    share = rank // fs
    tokens = out_cot.shape[0]
    rows = inner // chunks
    entries = float(width * fs * inner * tp)
    part = lax.rem(mine, PARTS)
    piece = 2 * rank // PARTS

    loads = []

    def fetch(src, dst):
        copy = pltpu.make_async_copy(src, dst, load.at[len(loads)])
        copy.start()
        loads.append(copy)
        return copy

    in_factor = [
        fetch(factor_out, full.at[me, pl.ds(0, rank)]),
        fetch(factor_z, full.at[me, pl.ds(rank, rank)]),
    ]
    in_weight = [fetch(weight_out, wo_v), fetch(weight_z, wz_v)]

    barrier = pltpu.get_barrier_semaphore()
    for d in range(1, fs):
        pl.semaphore_signal(barrier, inc=1, device_id={"fs": lax.rem(me + d, fs)}, device_id_type=MESH)
    for d in range(1, tp):
        pl.semaphore_signal(barrier, inc=1, device_id={"tp": lax.rem(mine + d, tp)}, device_id_type=MESH)
    for copy in in_factor:
        copy.wait()
    pl.semaphore_wait(barrier, fs + tp - 2)

    def piece_of(src, p):
        return full.at[src, pl.ds(pl.multiple_of(p * piece, piece), piece)]

    spread = []
    for d in range(1, fs):
        block = piece_of(me, part)
        copy = remote(block, block, send_f.at[d - 1], recv_f.at[d - 1], fs=lax.rem(me + d, fs))
        copy.start()
        spread.append(copy)

    for copy in in_weight:
        copy.wait()
    in_tokens = [
        (fetch(out_cot, tokens_v.at[0]), fetch(gated, inner_v.at[0])),
        (fetch(block_in, tokens_v.at[1]), fetch(gate, inner_v.at[1])),
    ]
    in_moments = [
        fetch(ref, moments_v.at[i]) for i, ref in enumerate((first_out, first_z, second_out, second_z))
    ]
    wt_v[...] = wz_v[...].T

    def chunk_of(src, c):
        return wall.at[src, pl.ds(pl.multiple_of(c * rows, rows), rows)]

    def up(h, c):
        block = chunk_of(jnp.maximum(me - h, 0), c)
        return remote(block, block, send_u.at[h, c], recv_u.at[h, c], fs=jnp.minimum(me + 1, fs - 1))

    def down(h, c):
        block = chunk_of(jnp.minimum(me + h, fs - 1), c)
        return remote(block, block, send_d.at[h, c], recv_d.at[h, c], fs=jnp.maximum(me - 1, 0))

    def start_own(c):
        @pl.when(me < fs - 1)
        def _():
            up(0, c).start()

        @pl.when(me > 0)
        def _():
            down(0, c).start()

    def pack(c, _):
        at = pl.ds(pl.multiple_of(c * rows, rows), rows)
        pair = jnp.concatenate([wo_v[at, :], wt_v[at, :]], axis=1)
        wall[me, at, :] = encode(pair, WEIGHT_BOUND, 1)

        @pl.when(c > 0)
        def _():
            start_own(c - 1)

        return 0

    lax.fori_loop(0, chunks, pack, 0)
    start_own(chunks - 1)

    def pump(h, low, high, rising=True, falling=True):
        def body(c, _):
            @pl.when((me - h >= 0) & (me < fs - 1) & rising)
            def _():
                up(h - 1, c).wait_recv()
                up(h, c).start()

            @pl.when((me + h < fs) & (me > 0) & falling)
            def _():
                down(h - 1, c).wait_recv()
                down(h, c).start()

            return 0

        lax.fori_loop(low, high, body, 0)

    plane = []

    def pass_on(d, k, p, bit):
        block = piece_of(lax.rem(me - d + fs, fs), p)
        copy = remote(block, block, send_p.at[d - 1, k], recv_p.at[d - 1, k], tp=flip(mine, bit))
        copy.start()
        plane.append(copy)
        return copy

    by_y, by_x = [], []
    for d in range(1, fs):
        spread[d - 1].wait_recv()
        by_y.append(pass_on(d, 0, part, 4))
        by_x.append([pass_on(d, 1, part, 2)])
        pass_on(d, 3, part, 1)
    for d in range(1, fs):
        by_y[d - 1].wait_recv()
        by_x[d - 1].append(pass_on(d, 2, flip(part, 4), 2))
        pass_on(d, 4, flip(part, 4), 1)
    for d in range(1, fs):
        for k, copy in enumerate(by_x[d - 1]):
            copy.wait_recv()
            p = flip(part, 2)
            pass_on(d, 5 + k, p if k == 0 else flip(p, 4), 1)
    waited = [c for c in by_y] + [c for pair in by_x for c in pair]
    for copy in plane:
        if not any(copy is other for other in waited):
            copy.wait_recv()

    block_t = 256 if tokens % 256 == 0 else tokens
    for m in range(2):
        joined[m] = jnp.concatenate(
            [full[s, pl.ds(m * rank, rank), :] for s in range(fs)], axis=1
        )
        for copy in in_tokens[m]:
            copy.wait()

        def project(c, _, m=m):
            at = pl.ds(pl.multiple_of(c * block_t, block_t), block_t)
            high, low = split(nt(joined[m], tokens_v[m, at, :]))
            other = inner_v[m, :, at]
            value = nt(high, other) + nt(low, other)
            term[m] = jnp.where(c == 0, value, term[m] + value)
            return 0

        term[m] = jnp.zeros((rank, inner), f32)
        lax.fori_loop(0, tokens // block_t, project, 0)

    half = chunks // 2 + 1
    upper = me * 2 >= fs
    lower = me * 2 < fs
    if fs > 2:
        pump(1, 0, half, upper, lower)

    def rise(t):
        return remote(
            rise_out.at[t - 1], rise_in.at[t - 1], send_r.at[0, t - 1], recv_r.at[0, t - 1],
            fs=jnp.minimum(me + 1, fs - 1),
        )

    def fall(t):
        return remote(
            fall_out.at[t], fall_in.at[t], send_r.at[1, t], recv_r.at[1, t], fs=jnp.maximum(me - 1, 0)
        )

    def link(t, first_one, made, move, out, came, slot):
        at = pl.ds(t * share, share)

        @pl.when(first_one)
        def _():
            out[slot] = encode(jnp.concatenate([term[0, at, :], term[1, at, :]], axis=1), grad_bound, 4)
            move(t).start()

        @pl.when(made)
        def _():
            move(t).wait_recv()
            value = jnp.concatenate([term[0, at, :], term[1, at, :]], axis=1)
            out[slot] = encode(value + decode(came[slot], grad_bound, 4), grad_bound, 4)
            move(t).start()

    for k in range(fs - 1):
        t = fs - 1 - k
        link(t, me == 0, (me > 0) & (me < t), rise, rise_out, rise_in, t - 1)
        link(k, me == fs - 1, (me < fs - 1) & (me > k), fall, fall_out, fall_in, k)
    for copy in in_moments:
        copy.wait()
    own = pl.ds(pl.multiple_of(me * share, share), share)
    sum_v[...] = jnp.concatenate([term[0, own, :], term[1, own, :]], axis=1)

    @pl.when(me > 0)
    def _():
        rise(me).wait_recv()
        sum_v[...] += decode(rise_in[me - 1], grad_bound, 4)

    @pl.when(me < fs - 1)
    def _():
        fall(me).wait_recv()
        sum_v[...] += decode(fall_in[me], grad_bound, 4)

    gradient = sum_v[...]
    first = jnp.concatenate([moments_v[0], moments_v[1]], axis=1)
    second = jnp.concatenate([moments_v[2], moments_v[3]], axis=1)
    moment = beta_first * first + (1.0 - beta_first) * gradient
    square = beta_second * second + (1.0 - beta_second) * gradient * gradient
    dir_code[me] = encode(moment / (jnp.sqrt(square) + adam_eps), DIR_BOUND, 3)
    new_first_out[...] = moment[:, :inner]
    new_first_z[...] = moment[:, inner:]
    new_second_out[...] = square[:, :inner]
    new_second_z[...] = square[:, inner:]
    gathers = []
    for d in range(1, fs):
        block = dir_code.at[me]
        copy = remote(block, block, send_g.at[d - 1], recv_g.at[d - 1], fs=lax.rem(me + d, fs))
        copy.start()
        gathers.append(copy)
    if fs > 2:
        pump(1, half, chunks, upper, lower)
        pump(1, 0, chunks, lower, upper)
    few = chunks // 6
    if fs > 3:
        pump(2, 0, few)
    for copy in gathers:
        copy.wait_recv()

    whole = decode(jnp.concatenate([dir_code[s] for s in range(fs)], axis=0), DIR_BOUND, 3)
    for m in range(2):
        values = whole[:, m * inner:(m + 1) * inner]
        high, low = split(values.T)
        dir_t[m, 0] = high
        dir_t[m, 1] = low
    high, low = split(whole[:, inner:])
    dir_n[0] = high
    dir_n[1] = low

    tall = inner // 3 if inner % 48 == 0 else inner
    squares = []
    for m in range(2):
        def grow(c, acc, m=m):
            at = pl.ds(pl.multiple_of(c * tall, tall), tall)
            value = nn(dir_t[m, 0, at, :], joined[m]) + nn(dir_t[m, 1, at, :], joined[m])
            update[m, at, :] = value
            return acc + jnp.sum(value * value, axis=0, keepdims=True)

        acc = lax.fori_loop(0, inner // tall, grow, jnp.zeros((1, fs * width), f32))
        squares.append(jnp.sum(acc))
    row = lax.broadcasted_iota(jnp.int32, partial.shape, 0)
    partial[...] = jnp.where(row == 0, squares[0], squares[1])
    own_z = full[me, pl.ds(rank, rank), :]
    step_z[...] = tn(own_z, dir_n[0]) + tn(own_z, dir_n[1])
    totals = []
    for d in range(1, tp):
        copy = remote(
            partial, received.at[d - 1], send_t.at[d - 1], recv_t.at[d - 1], tp=lax.rem(mine + d, tp)
        )
        copy.start()
        totals.append(copy)
    own_out = full[me, pl.ds(0, rank), :]
    step_out[...] = nn(dir_t[0, 0], own_out) + nn(dir_t[0, 1], own_out)
    if fs > 3:
        pump(2, few, chunks)
    for h in range(3, fs - 1):
        pump(h, 0, chunks)
    result = partial[...]
    for d in range(1, tp):
        totals[d - 1].wait_recv()
        result = result + received[d - 1]
    scale = lax.rsqrt(result * (1.0 / entries) + norm_eps)
    scale_out, scale_z = scale[0:1, 0:1], scale[1:2, 0:1]
    step_out[...] = step_out[...] * scale_out
    step_z[...] = step_z[...] * scale_z

    def finish(c, _):
        @pl.when(me == fs - 1)
        def _():
            for h in range(fs - 1):
                up(h, c).wait_recv()

        @pl.when(me == 0)
        def _():
            for h in range(fs - 1):
                down(h, c).wait_recv()

        def fresh(r, _):
            at = pl.ds(pl.multiple_of(c * rows + r * 16, 16), 16)
            for m, (dst, size) in enumerate(((copy_out, scale_out), (copy_z, scale_z))):
                code = jnp.concatenate(
                    [wall[s, at, m * width:(m + 1) * width] for s in range(fs)], axis=1
                )
                step = update[m, at, :] * size
                dst[at, :] = (decode(code, WEIGHT_BOUND, 1) - rate * step).astype(bf16)
            return 0

        lax.fori_loop(0, rows // 16, fresh, 0)
        return 0

    lax.fori_loop(0, chunks, finish, 0)

    for h in range(fs - 1):
        def drain(c, _, h=h):
            @pl.when((me - h >= 0) & (me < fs - 1))
            def _():
                up(h, c).wait_send()

            @pl.when((me + h < fs) & (me > 0))
            def _():
                down(h, c).wait_send()

            return 0

        lax.fori_loop(0, chunks, drain, 0)
    for k in range(fs - 1):
        t = fs - 1 - k

        @pl.when(me < t)
        def _(t=t):
            rise(t).wait_send()

        @pl.when(me > k)
        def _(k=k):
            fall(k).wait_send()

    for copy in spread + plane + gathers + totals:
        copy.wait_send()


def store_kernel(*refs):
    count = (len(refs) - 1) // 2
    sems = refs[-1]
    copies = [
        pltpu.make_async_copy(refs[i], refs[count + i], sems.at[i]) for i in range(count)
    ]
    for copy in copies:
        copy.start()
    for copy in copies:
        copy.wait()


def per_device(
    fs, tp,
    block_in, out_cot, gated_out, gate_cot, factor_out, factor_z,
    weight_out, weight_z, first_out, second_out, first_z, second_z,
):
    width, rank = factor_out.shape
    tokens, inner = gated_out.shape
    share = rank // fs
    chunks = next(n for n in (12, 6, 3, 2, 1) if inner % (16 * n) == 0)
    grad_bound = 2.0 ** math.ceil(
        math.log2(tokens * VALUE_BOUND * width * fs * VALUE_BOUND * FACTOR_BOUND)
    )
    dma = pltpu.SemaphoreType.DMA
    shape = jax.ShapeDtypeStruct
    moment = shape((share, inner), f32)
    results = (
        shape((inner, fs * width), bf16),
        shape((inner, fs * width), bf16),
        shape((inner, width), f32),
        shape((width, inner), f32),
        moment, moment, moment, moment,
    )
    hops = dma((fs - 1, chunks))
    peers = dma((fs - 1,))
    chain = dma((2, fs - 1))
    others = dma((tp - 1,))
    pieces = dma((fs - 1, PARTS - 1))
    made = pl.pallas_call(
        functools.partial(main_kernel, fs, tp, chunks, grad_bound),
        out_shape=tuple(pltpu.VMEM(r.shape, r.dtype) for r in results),
        in_specs=[ANY] * 12,
        out_specs=[VMEM] * 8,
        scratch_shapes=[
            pltpu.VMEM((2, tokens, fs * width), bf16),
            pltpu.VMEM((2, inner, tokens), bf16),
            pltpu.VMEM((inner, width), f32),
            pltpu.VMEM((width, inner), f32),
            pltpu.VMEM((inner, width), f32),
            pltpu.VMEM((4, share, inner), f32),
            pltpu.VMEM((fs, 2 * rank, width), bf16),
            pltpu.VMEM((fs, inner, 2 * width), bf16),
            pltpu.VMEM((2, rank, fs * width), bf16),
            pltpu.VMEM((2, rank, inner), f32),
            pltpu.VMEM((fs - 1, share, 2 * inner), bf16),
            pltpu.VMEM((fs - 1, share, 2 * inner), bf16),
            pltpu.VMEM((fs - 1, share, 2 * inner), bf16),
            pltpu.VMEM((fs - 1, share, 2 * inner), bf16),
            pltpu.VMEM((share, 2 * inner), f32),
            pltpu.VMEM((fs, share, 2 * inner), bf16),
            pltpu.VMEM((2, 2, inner, rank), bf16),
            pltpu.VMEM((2, rank, inner), bf16),
            pltpu.VMEM((2, inner, fs * width), f32),
            pltpu.VMEM((8, 128), f32),
            pltpu.VMEM((tp - 1, 8, 128), f32),
            dma((12,)),
            peers, peers, pieces, pieces, hops, hops, hops, hops,
            chain, chain, peers, peers, others, others,
        ],
        compiler_params=pltpu.CompilerParams(
            collective_id=0, has_side_effects=True, vmem_limit_bytes=48 * 1024 * 1024
        ),
        cost_estimate=pl.CostEstimate(flops=10**10, bytes_accessed=30_000_000, transcendentals=0),
    )(*[pltpu.with_memory_space_constraint(v, pltpu.HBM) for v in (
        out_cot, block_in, gated_out.T, gate_cot.T, factor_out.T, factor_z.T, weight_out, weight_z,
        first_out.T, second_out.T, first_z, second_z,
    )])
    kept = pl.pallas_call(
        store_kernel,
        out_shape=results,
        in_specs=[VMEM] * 8,
        out_specs=[ANY] * 8,
        scratch_shapes=[dma((8,))],
        compiler_params=pltpu.CompilerParams(vmem_limit_bytes=1024 * 1024),
        cost_estimate=pl.CostEstimate(flops=10**6, bytes_accessed=20_000_000, transcendentals=0),
    )(*[pltpu.with_memory_space_constraint(v, pltpu.VMEM) for v in made])
    copy_out, copy_z, step_out, step_z, nf_out, ns_out, nf_z, ns_z = kept
    return step_out, step_z, nf_out.T, ns_out.T, nf_z, ns_z, copy_out, copy_z.T


def solution(mesh):
    return jax.shard_map(
        functools.partial(per_device, mesh.shape["fs"], mesh.shape["tp"]),
        mesh=mesh,
        in_specs=(
            P("fs", None),
            P("fs", None),
            P("fs", "tp"),
            P("fs", "tp"),
            P("fs", None),
            P("fs", None),
            P("tp", "fs"),
            P("fs", "tp"),
            P("tp", "fs"),
            P("tp", "fs"),
            P("fs", "tp"),
            P("fs", "tp"),
        ),
        out_specs=(
            P("tp", "fs"),
            P("fs", "tp"),
            P("tp", "fs"),
            P("tp", "fs"),
            P("fs", "tp"),
            P("fs", "tp"),
            P("tp", None),
            P(None, "tp"),
        ),
        check_vma=False,
    )
```

```python
import functools
import math

import jax
import jax.numpy as jnp
from jax import lax
from jax.experimental import pallas as pl
from jax.experimental.pallas import tpu as pltpu
from jax.sharding import PartitionSpec as P

beta_first = 0.8
beta_second = 0.9
adam_eps = 1e-08
norm_eps = 1e-06
rate = 0.005

MESH = pl.DeviceIdType.MESH
VMEM = pl.BlockSpec(memory_space=pltpu.VMEM)
ANY = pl.BlockSpec(memory_space=pl.ANY)
PARTS = 8
SPAN = 120.0 * math.log(2.0)
WEIGHT_BOUND = 0.125
DIR_BOUND = 16.0
VALUE_BOUND = 6.0
FACTOR_BOUND = 0.104166667

f32, bf16 = jnp.float32, jnp.bfloat16


def remote(src, dst, send, recv, **where):
    return pltpu.make_async_remote_copy(
        src_ref=src, dst_ref=dst, send_sem=send, recv_sem=recv, device_id=where, device_id_type=MESH
    )


def encode(values, bound, roots):
    size = jnp.abs(values) * (1.0 / bound)
    for _ in range(roots):
        size = jnp.sqrt(size)
    code = jnp.exp(size * (2.0 * SPAN) - SPAN)
    return jnp.where(values < 0.0, -code, code).astype(bf16)


def decode(code, bound, roots):
    code = code.astype(f32)
    size = (jnp.log(jnp.abs(code)) + SPAN) * (0.5 / SPAN)
    for _ in range(roots):
        size = size * size
    size = size * bound
    return jnp.where(code < 0.0, -size, size)


def split(values):
    high = values.astype(bf16)
    return high, (values - high.astype(f32)).astype(bf16)


def nn(a, b):
    return jnp.dot(a, b, preferred_element_type=f32)


def nt(a, b):
    return lax.dot_general(a, b, (((1,), (1,)), ((), ())), preferred_element_type=f32)


def tn(a, b):
    return lax.dot_general(a, b, (((0,), (0,)), ((), ())), preferred_element_type=f32)


def flip(index, bit):
    return index + bit - 2 * bit * lax.rem(index // bit, 2)


def cut(total):
    sizes = []
    while total:
        sizes.append(-(-total // 3))
        total -= sizes[-1]
    return sizes


def main_kernel(
    fs, tp, sizes, grad_bound,
    out_cot, block_in, gated, gate, factor_out, factor_z, weight_out, weight_z,
    first_out, second_out, first_z, second_z,
    copy_out, copy_z, step_out, step_z, new_first_out, new_second_out, new_first_z, new_second_z,
    tokens_v, inner_v, wo_v, wz_v, wt_v, moments_v,
    full, wall, joined, term, rise_out, rise_in, fall_out, fall_in, sum_v, dir_code, dir_t, dir_n, update,
    partial, received,
    load, send_f, recv_f, send_p, recv_p, send_u, recv_u, send_d, recv_d,
    send_r, recv_r, send_g, recv_g, send_t, recv_t,
):
    me, mine = lax.axis_index("fs"), lax.axis_index("tp")
    inner, width = weight_out.shape
    rank = factor_out.shape[0]
    share = rank // fs
    tokens = out_cot.shape[0]
    chunks = len(sizes)
    starts = [sum(sizes[:c]) for c in range(chunks)]
    entries = float(width * fs * inner * tp)
    part = lax.rem(mine, PARTS)
    piece = 2 * rank // PARTS

    barrier = pltpu.get_barrier_semaphore()
    for d in range(1, fs):
        pl.semaphore_signal(barrier, inc=1, device_id={"fs": lax.rem(me + d, fs)}, device_id_type=MESH)
    for d in range(1, tp):
        pl.semaphore_signal(barrier, inc=1, device_id={"tp": lax.rem(mine + d, tp)}, device_id_type=MESH)

    def fetch(src, dst, k):
        copy = pltpu.make_async_copy(src, dst, load.at[k])
        copy.start()
        return copy

    fetch(factor_out, full.at[me, pl.ds(0, rank)], 0)
    fetch(factor_z, full.at[me, pl.ds(rank, rank)], 0)
    in_weight = [fetch(weight_out, wo_v, 1), fetch(weight_z, wz_v, 2)]
    pltpu.make_async_copy(full.at[me], full.at[me], load.at[0]).wait()
    pl.semaphore_wait(barrier, fs + tp - 2)

    def piece_of(src, p):
        return full.at[src, pl.ds(pl.multiple_of(p * piece, piece), piece)]

    spread = []
    for d in range(1, fs):
        block = piece_of(me, part)
        copy = remote(block, block, send_f.at[d - 1], recv_f.at[d - 1], fs=lax.rem(me + d, fs))
        copy.start()
        spread.append(copy)

    for copy in in_weight:
        copy.wait()
    in_tokens = [
        (fetch(out_cot, tokens_v.at[0], 3), fetch(gated, inner_v.at[0], 4)),
        (fetch(block_in, tokens_v.at[1], 5), fetch(gate, inner_v.at[1], 6)),
    ]
    for i, ref in enumerate((first_out, first_z, second_out, second_z)):
        fetch(ref, moments_v.at[i], 7)
    wt_v[...] = wz_v[...].T

    def chunk_of(src, c):
        return wall.at[src, pl.ds(starts[c], sizes[c])]

    def up(h, c):
        block = chunk_of(jnp.maximum(me - h, 0), c)
        return remote(block, block, send_u.at[h], recv_u.at[h, c], fs=jnp.minimum(me + 1, fs - 1))

    def down(h, c):
        block = chunk_of(jnp.minimum(me + h, fs - 1), c)
        return remote(block, block, send_d.at[h], recv_d.at[h, c], fs=jnp.maximum(me - 1, 0))

    late = lax.rem(mine, 2) == 1

    def start_own(c, now):
        @pl.when((me < fs - 1) & now)
        def _():
            up(0, c).start()

        @pl.when((me > 0) & now)
        def _():
            down(0, c).start()

    def pack(r, _):
        at = pl.ds(pl.multiple_of(r * 16, 16), 16)
        pair = jnp.concatenate([wo_v[at, :], wt_v[at, :]], axis=1)
        wall[me, at, :] = encode(pair, WEIGHT_BOUND, 1)
        return 0

    for c in range(chunks):
        lax.fori_loop(starts[c] // 16, (starts[c] + sizes[c]) // 16, pack, 0)
        if c:
            start_own(c - 1, ~late)
    start_own(chunks - 1, ~late)

    def pump(h, low, high, rising=True, falling=True):
        for c in range(low, high):
            @pl.when((me - h >= 0) & (me < fs - 1) & rising)
            def _(c=c):
                up(h - 1, c).wait_recv()
                up(h, c).start()

            @pl.when((me + h < fs) & (me > 0) & falling)
            def _(c=c):
                down(h - 1, c).wait_recv()
                down(h, c).start()

    def pass_on(d, p, bit, k):
        block = piece_of(lax.rem(me - d + fs, fs), p)
        copy = remote(block, block, send_p.at[d - 1], recv_p.at[d - 1, k], tp=flip(mine, bit))
        copy.start()
        return copy

    by_y, by_x = [], []
    for d in range(1, fs):
        spread[d - 1].wait_recv()
        by_y.append(pass_on(d, part, 4, 0))
        by_x.append([pass_on(d, part, 2, 1)])
        pass_on(d, part, 1, 3)
    for d in range(1, fs):
        by_y[d - 1].wait_recv()
        by_x[d - 1].append(pass_on(d, flip(part, 4), 2, 2))
        pass_on(d, flip(part, 4), 1, 3)
    for c in range(chunks):
        start_own(c, late)
    for d in range(1, fs):
        for k, copy in enumerate(by_x[d - 1]):
            copy.wait_recv()
            p = flip(part, 2)
            pass_on(d, p if k == 0 else flip(p, 4), 1, 3)
    for d in range(1, fs):
        block = full.at[0, pl.ds(0, 4 * piece)]
        remote(block, block, send_p.at[d - 1], recv_p.at[d - 1, 3], tp=flip(mine, 1)).wait_recv()

    block_t = 256 if tokens % 256 == 0 else tokens
    for m in range(2):
        joined[m] = jnp.concatenate(
            [full[s, pl.ds(m * rank, rank), :] for s in range(fs)], axis=1
        )
        for copy in in_tokens[m]:
            copy.wait()

        def project(c, _, m=m):
            at = pl.ds(pl.multiple_of(c * block_t, block_t), block_t)
            high, low = split(nt(joined[m], tokens_v[m, at, :]))
            other = inner_v[m, :, at]
            value = nt(high, other) + nt(low, other)
            term[m] = jnp.where(c == 0, value, term[m] + value)
            return 0

        term[m] = jnp.zeros((rank, inner), f32)
        lax.fori_loop(0, tokens // block_t, project, 0)

    half = 2
    upper = me * 2 >= fs
    lower = me * 2 < fs
    if fs > 2:
        pump(1, 0, half, upper, lower)

    def rise(t):
        return remote(
            rise_out.at[t - 1], rise_in.at[t - 1], send_r.at[0, t - 1], recv_r.at[0, t - 1],
            fs=jnp.minimum(me + 1, fs - 1),
        )

    def fall(t):
        return remote(
            fall_out.at[t], fall_in.at[t], send_r.at[1, t], recv_r.at[1, t], fs=jnp.maximum(me - 1, 0)
        )

    def link(t, first_one, made, move, out, came, slot):
        at = pl.ds(t * share, share)

        @pl.when(first_one)
        def _():
            out[slot] = encode(jnp.concatenate([term[0, at, :], term[1, at, :]], axis=1), grad_bound, 4)
            move(t).start()

        @pl.when(made)
        def _():
            move(t).wait_recv()
            value = jnp.concatenate([term[0, at, :], term[1, at, :]], axis=1)
            out[slot] = encode(value + decode(came[slot], grad_bound, 4), grad_bound, 4)
            move(t).start()

    for k in range(fs - 1):
        t = fs - 1 - k
        link(t, me == 0, (me > 0) & (me < t), rise, rise_out, rise_in, t - 1)
        link(k, me == fs - 1, (me < fs - 1) & (me > k), fall, fall_out, fall_in, k)
    pltpu.make_async_copy(moments_v, moments_v, load.at[7]).wait()
    own = pl.ds(pl.multiple_of(me * share, share), share)
    sum_v[...] = jnp.concatenate([term[0, own, :], term[1, own, :]], axis=1)

    @pl.when(me > 0)
    def _():
        rise(me).wait_recv()
        sum_v[...] += decode(rise_in[me - 1], grad_bound, 4)

    @pl.when(me < fs - 1)
    def _():
        fall(me).wait_recv()
        sum_v[...] += decode(fall_in[me], grad_bound, 4)

    gradient = sum_v[...]
    first = jnp.concatenate([moments_v[0], moments_v[1]], axis=1)
    second = jnp.concatenate([moments_v[2], moments_v[3]], axis=1)
    moment = beta_first * first + (1.0 - beta_first) * gradient
    square = beta_second * second + (1.0 - beta_second) * gradient * gradient
    dir_code[me] = encode(moment / (jnp.sqrt(square) + adam_eps), DIR_BOUND, 3)
    new_first_out[...] = moment[:, :inner]
    new_first_z[...] = moment[:, inner:]
    new_second_out[...] = square[:, :inner]
    new_second_z[...] = square[:, inner:]
    for d in range(1, fs):
        block = dir_code.at[me]
        remote(block, block, send_g.at[0], recv_g.at[0], fs=lax.rem(me + d, fs)).start()
    if fs > 2:
        pump(1, half, chunks, upper, lower)
        pump(1, 0, chunks, lower, upper)
    few = 1
    if fs > 3:
        pump(2, 0, few)
    block = dir_code.at[pl.ds(0, fs - 1)]
    gathers = remote(block, block, send_g.at[0], recv_g.at[0], fs=lax.rem(me + 1, fs))
    gathers.wait_recv()

    whole = decode(jnp.concatenate([dir_code[s] for s in range(fs)], axis=0), DIR_BOUND, 3)
    for m in range(2):
        values = whole[:, m * inner:(m + 1) * inner]
        high, low = split(values.T)
        dir_t[m, 0] = high
        dir_t[m, 1] = low
    high, low = split(whole[:, inner:])
    dir_n[0] = high
    dir_n[1] = low

    tall = inner // 3 if inner % 48 == 0 else inner
    squares = []
    for m in range(2):
        def grow(c, acc, m=m):
            at = pl.ds(pl.multiple_of(c * tall, tall), tall)
            value = nn(dir_t[m, 0, at, :], joined[m]) + nn(dir_t[m, 1, at, :], joined[m])
            update[m, at, :] = value
            return acc + jnp.sum(value * value, axis=0, keepdims=True)

        acc = lax.fori_loop(0, inner // tall, grow, jnp.zeros((1, fs * width), f32))
        squares.append(jnp.sum(acc))
    row = lax.broadcasted_iota(jnp.int32, partial.shape, 0)
    partial[...] = jnp.where(row == 0, squares[0], squares[1])
    own_z = full[me, pl.ds(rank, rank), :]
    step_z[...] = tn(own_z, dir_n[0]) + tn(own_z, dir_n[1])
    for d in range(1, tp):
        remote(partial, received.at[d - 1], send_t.at[0], recv_t.at[0], tp=lax.rem(mine + d, tp)).start()
    own_out = full[me, pl.ds(0, rank), :]
    step_out[...] = nn(dir_t[0, 0], own_out) + nn(dir_t[0, 1], own_out)
    if fs > 3:
        pump(2, few, chunks)
    for h in range(3, fs - 1):
        pump(h, 0, chunks)
    result = partial[...]
    totals = remote(received, received, send_t.at[0], recv_t.at[0], tp=lax.rem(mine + 1, tp))
    totals.wait_recv()
    for d in range(1, tp):
        result = result + received[d - 1]
    scale = lax.rsqrt(result * (1.0 / entries) + norm_eps)
    scale_out, scale_z = scale[0:1, 0:1], scale[1:2, 0:1]
    step_out[...] = step_out[...] * scale_out
    step_z[...] = step_z[...] * scale_z

    def drain(ends):
        for h in range(fs - 1):
            @pl.when((me - h >= 0) & (me < fs - 1) & ends)
            def _(h=h):
                block = wall.at[0]
                remote(block, block, send_u.at[h], recv_u.at[h, 0], fs=jnp.minimum(me + 1, fs - 1)).wait_send()

            @pl.when((me + h < fs) & (me > 0) & ends)
            def _(h=h):
                block = wall.at[0]
                remote(block, block, send_d.at[h], recv_d.at[h, 0], fs=jnp.maximum(me - 1, 0)).wait_send()

    outer = (me == 0) | (me == fs - 1)
    drain(outer)
    block = full.at[0, pl.ds(0, (PARTS - 1) * piece)]
    for d in range(1, fs):
        remote(block, block, send_p.at[d - 1], recv_p.at[d - 1, 3], tp=flip(mine, 1)).wait_send()
    for copy in spread:
        copy.wait_send()
    gathers.wait_send()
    totals.wait_send()
    for k in range(fs - 1):
        t = fs - 1 - k

        @pl.when(me < t)
        def _(t=t):
            rise(t).wait_send()

        @pl.when(me > k)
        def _(k=k):
            fall(k).wait_send()

    def fresh(r, _):
        at = pl.ds(pl.multiple_of(r * 16, 16), 16)
        for m, (dst, size) in enumerate(((copy_out, scale_out), (copy_z, scale_z))):
            code = jnp.concatenate(
                [wall[s, at, m * width:(m + 1) * width] for s in range(fs)], axis=1
            )
            step = update[m, at, :] * size
            dst[at, :] = (decode(code, WEIGHT_BOUND, 1) - rate * step).astype(bf16)
        return 0

    for c in range(chunks):
        @pl.when(me == fs - 1)
        def _(c=c):
            for h in range(fs - 1):
                up(h, c).wait_recv()

        @pl.when(me == 0)
        def _(c=c):
            for h in range(fs - 1):
                down(h, c).wait_recv()

        lax.fori_loop(starts[c] // 16, (starts[c] + sizes[c]) // 16, fresh, 0)

    drain((me > 0) & (me < fs - 1))


def store_kernel(*refs):
    count = (len(refs) - 1) // 2
    sems = refs[-1]
    copies = [
        pltpu.make_async_copy(refs[i], refs[count + i], sems.at[i]) for i in range(count)
    ]
    for copy in copies:
        copy.start()
    for copy in copies:
        copy.wait()


def per_device(
    fs, tp,
    block_in, out_cot, gated_out, gate_cot, factor_out, factor_z,
    weight_out, weight_z, first_out, second_out, first_z, second_z,
):
    width, rank = factor_out.shape
    tokens, inner = gated_out.shape
    share = rank // fs
    sizes = [16 * n for n in cut(inner // 16)]
    chunks = len(sizes)
    grad_bound = 2.0 ** math.ceil(
        math.log2(tokens * VALUE_BOUND * width * fs * VALUE_BOUND * FACTOR_BOUND)
    )
    dma = pltpu.SemaphoreType.DMA
    shape = jax.ShapeDtypeStruct
    moment = shape((share, inner), f32)
    results = (
        shape((inner, fs * width), bf16),
        shape((inner, fs * width), bf16),
        shape((inner, width), f32),
        shape((width, inner), f32),
        moment, moment, moment, moment,
    )
    hops = dma((fs - 1, chunks))
    peers = dma((fs - 1,))
    chain = dma((2, fs - 1))
    single = dma((1,))
    pieces = dma((fs - 1, 4))
    made = pl.pallas_call(
        functools.partial(main_kernel, fs, tp, sizes, grad_bound),
        out_shape=tuple(pltpu.VMEM(r.shape, r.dtype) for r in results),
        in_specs=[ANY] * 12,
        out_specs=[VMEM] * 8,
        scratch_shapes=[
            pltpu.VMEM((2, tokens, fs * width), bf16),
            pltpu.VMEM((2, inner, tokens), bf16),
            pltpu.VMEM((inner, width), f32),
            pltpu.VMEM((width, inner), f32),
            pltpu.VMEM((inner, width), f32),
            pltpu.VMEM((4, share, inner), f32),
            pltpu.VMEM((fs, 2 * rank, width), bf16),
            pltpu.VMEM((fs, inner, 2 * width), bf16),
            pltpu.VMEM((2, rank, fs * width), bf16),
            pltpu.VMEM((2, rank, inner), f32),
            pltpu.VMEM((fs - 1, share, 2 * inner), bf16),
            pltpu.VMEM((fs - 1, share, 2 * inner), bf16),
            pltpu.VMEM((fs - 1, share, 2 * inner), bf16),
            pltpu.VMEM((fs - 1, share, 2 * inner), bf16),
            pltpu.VMEM((share, 2 * inner), f32),
            pltpu.VMEM((fs, share, 2 * inner), bf16),
            pltpu.VMEM((2, 2, inner, rank), bf16),
            pltpu.VMEM((2, rank, inner), bf16),
            pltpu.VMEM((2, inner, fs * width), f32),
            pltpu.VMEM((8, 128), f32),
            pltpu.VMEM((tp - 1, 8, 128), f32),
            dma((8,)),
            peers, peers, peers, pieces, peers, hops, peers, hops,
            chain, chain, single, single, single, single,
        ],
        compiler_params=pltpu.CompilerParams(
            collective_id=0, has_side_effects=True, vmem_limit_bytes=48 * 1024 * 1024
        ),
        cost_estimate=pl.CostEstimate(flops=10**10, bytes_accessed=30_000_000, transcendentals=0),
    )(*[pltpu.with_memory_space_constraint(v, pltpu.HBM) for v in (
        out_cot, block_in, gated_out.T, gate_cot.T, factor_out.T, factor_z.T, weight_out, weight_z,
        first_out.T, second_out.T, first_z, second_z,
    )])
    kept = pl.pallas_call(
        store_kernel,
        out_shape=results,
        in_specs=[VMEM] * 8,
        out_specs=[ANY] * 8,
        scratch_shapes=[dma((8,))],
        compiler_params=pltpu.CompilerParams(vmem_limit_bytes=1024 * 1024),
        cost_estimate=pl.CostEstimate(flops=10**6, bytes_accessed=20_000_000, transcendentals=0),
    )(*[pltpu.with_memory_space_constraint(v, pltpu.VMEM) for v in made])
    copy_out, copy_z, step_out, step_z, nf_out, ns_out, nf_z, ns_z = kept
    return step_out, step_z, nf_out.T, ns_out.T, nf_z, ns_z, copy_out, copy_z.T


def solution(mesh):
    return jax.shard_map(
        functools.partial(per_device, mesh.shape["fs"], mesh.shape["tp"]),
        mesh=mesh,
        in_specs=(
            P("fs", None),
            P("fs", None),
            P("fs", "tp"),
            P("fs", "tp"),
            P("fs", None),
            P("fs", None),
            P("tp", "fs"),
            P("fs", "tp"),
            P("tp", "fs"),
            P("tp", "fs"),
            P("fs", "tp"),
            P("fs", "tp"),
        ),
        out_specs=(
            P("tp", "fs"),
            P("fs", "tp"),
            P("tp", "fs"),
            P("tp", "fs"),
            P("fs", "tp"),
            P("fs", "tp"),
            P("tp", None),
            P(None, "tp"),
        ),
        check_vma=False,
    )
```
